32 devices in a mesh: sp: 8 (over z, y), dp: 4 (over x, core).
Axes of the slice: x: 2, y: 2, z: 4, core: 2. Of those that a mesh axis runs over, the one named last changes fastest.
Arguments:
- queries: bfloat16 [16, 16, 512, 128], P('dp', None, 'sp'), may hold values from -6 to 6
- key_maps: bfloat16 [16, 16, 512, 128], P('dp', None, 'sp'), may hold values from -6 to 6
- value_rows: bfloat16 [16, 16, 512, 128], P('dp', None, 'sp'), may hold values from -6 to 6
- gate_logits: bfloat16 [512, 16, 2048], P('sp', 'dp'), may hold values from -6 to 6
- mix_lambda: float32 [16], replicated, may hold values from 0.3 to 0.8
- head_gain: float32 [128], replicated, may hold values from 0.1 to 1.9
- out_weight: bfloat16 [2048, 2048], P('sp', 'dp'), may hold values from -0.125 to 0.125
Outputs:
- projected: bfloat16 [512, 16, 2048], P('sp', 'dp')
The draws below stay inside these ranges and needn't reach their ends.
All inputs are finite; a program needn't handle non-finite values.
Results may differ from the reference program's by a relative error of at most 0.0075.
Values may be sent and summed in bfloat16 or wider, within the bound.
No kernel may reach another device: no remote copies, remote signals or barrier semaphores. Data moves between devices by JAX's collectives and lax.ppermute only.
A program may use at most 64 MiB of HBM per device.

```python
from functools import partial
import jax
import jax.numpy as jnp
from jax import lax

HEADS = 16
HEAD_DIM = 64
V_DIM = 128
STRETCH = 64
BLOCK = 512
D = 2048
LENGTH = 512
BATCH = 16


def draw_pair(key):
    shape = (BATCH, HEADS, LENGTH, 2 * HEAD_DIM)
    query_key = jax.random.fold_in(key, 11)
    keymap_key = jax.random.fold_in(key, 12)
    query_vals = jnp.clip(1.3 * jax.random.normal(query_key, shape, jnp.float32), -6.0, 6.0)
    keymap_vals = jnp.clip(1.3 * jax.random.normal(keymap_key, shape, jnp.float32), -6.0, 6.0)
    return (query_vals, keymap_vals)


def draw_queries(key, part):
    return draw_pair(key)[0].astype(jnp.bfloat16)


def draw_key_maps(key, part):
    return draw_pair(key)[1].astype(jnp.bfloat16)


def levels(stream_key, extent, shards, smallest, largest):
    factor_of, own = 1.0, jax.random.fold_in(stream_key, 6)
    for position, parts in shards:
        draws = jnp.exp(jax.random.uniform(jax.random.fold_in(own, position), (parts,), jnp.float32, smallest / len(shards), largest / len(shards)))
        factor_of = factor_of * jnp.repeat(draws, extent[position] // parts).reshape([-1 if axis == position else 1 for axis in range(len(extent))])
    return factor_of


def scatter_about(stream_key, shape, spread, reach, pieces=(), dtype=jnp.bfloat16):
    entries = spread * jax.random.normal(stream_key, shape, jnp.float32)
    if pieces:
        entries = entries * levels(stream_key, shape, pieces, -0.22, 0.18)
    return jnp.clip(entries, -reach, reach).astype(dtype)


def setup_inputs(seed: int = 0) -> dict:
    key_of = jax.random.split(jax.random.key(seed), 8)
    queries = draw_queries(jax.random.fold_in(key_of[7], 71), 0)
    key_maps = draw_key_maps(jax.random.fold_in(key_of[7], 71), 0)
    value_rows = scatter_about(key_of[2], (BATCH, HEADS, LENGTH, V_DIM), 1.0, 6.0, ((0, 4), (2, 8)))
    gate_logits = scatter_about(key_of[3], (LENGTH, BATCH, D), 1.0, 6.0, ((0, 8), (1, 4)))
    mix_lambda = jnp.clip(jax.random.uniform(key_of[4], (HEADS,), jnp.float32, 0.3, 0.8), 0.3, 0.8)
    head_gain = jnp.clip(1.0 + 0.18 * jax.random.normal(key_of[5], (V_DIM,), jnp.float32), 0.1, 1.9)
    out_weight = scatter_about(key_of[6], (D, D), D ** -0.5, 0.125, ((0, 8), (1, 4)))
    return dict(queries=queries, key_maps=key_maps, value_rows=value_rows, gate_logits=gate_logits, mix_lambda=mix_lambda, head_gain=head_gain, out_weight=out_weight)


def attend_item(operands, segment_ids, head_gain):
    query_item, key_item, value_item, weight_two = operands
    block_len = min(BLOCK, LENGTH)
    score_scale = HEAD_DIM ** (-0.5)
    outputs = []
    for block_index in range(LENGTH // block_len):
        offset = block_index * block_len
        limit = offset + block_len
        query_rows = query_item[offset:limit]
        key_block = key_item[:limit]
        value_block = value_item[:limit]
        visible = segment_ids[None, :limit] <= segment_ids[offset:limit, None]
        mapped = []
        for which in range(2):
            column_span = slice(which * HEAD_DIM, (which + 1) * HEAD_DIM)
            scores = jnp.dot(query_rows[:, column_span], key_block[:, column_span].T, preferred_element_type=jnp.float32) * score_scale
            scores = jnp.where(visible, scores, -1e+30)
            weights = jnp.exp(scores - lax.optimization_barrier(jnp.max(scores, axis=1, keepdims=True)))
            summed = lax.optimization_barrier(jnp.sum(weights, axis=1, keepdims=True))
            product = jnp.dot(weights.astype(jnp.bfloat16), value_block, preferred_element_type=jnp.float32)
            mapped.append(product / summed)
        combined = mapped[0] - weight_two * mapped[1]
        mean_sq = lax.optimization_barrier(jnp.mean(combined * combined, axis=1, keepdims=True))
        outputs.append((combined * lax.rsqrt(mean_sq + 1e-05) * head_gain).astype(jnp.bfloat16))
    return jnp.concatenate(outputs, axis=0)

def reference(queries, key_maps, value_rows, gate_logits, mix_lambda, head_gain, out_weight):
    item_count = BATCH * HEADS
    segment_ids = (jnp.arange(LENGTH) // STRETCH).astype(jnp.int32)
    lambda_items = jnp.tile(mix_lambda, BATCH)
    normed = lax.map(partial(attend_item, segment_ids=segment_ids, head_gain=head_gain), (queries.reshape(item_count, LENGTH, 2 * HEAD_DIM), key_maps.reshape(item_count, LENGTH, 2 * HEAD_DIM), value_rows.reshape(item_count, LENGTH, V_DIM), lambda_items))
    by_token = jnp.transpose(normed.reshape(BATCH, HEADS, LENGTH, V_DIM), (2, 0, 1, 3)).reshape(LENGTH, BATCH, D)
    gated = (jax.nn.sigmoid(gate_logits.astype(jnp.float32)) * by_token.astype(jnp.float32)).astype(jnp.bfloat16)
    output = jnp.dot(gated.reshape(LENGTH * BATCH, D), out_weight, preferred_element_type=jnp.float32)
    return output.astype(jnp.bfloat16).reshape(LENGTH, BATCH, D)
```

```python
import functools
import math

import jax
import jax.numpy as jnp
from jax import lax
from jax.experimental import pallas as pl
from jax.experimental.pallas import tpu as pltpu
from jax.sharding import PartitionSpec as P

STRETCH = 64
EPS = 1e-05
HIDDEN = -1e30
LOG2E = math.log2(math.e)


def contract_last(a, b):
    return lax.dot_general(a, b, (((1,), (1,)), ((), ())), preferred_element_type=jnp.float32)


def attend_kernel(place_ref, lam_ref, gain_ref, got_ref, out_ref):
    ranks, _, _, rows, cols = got_ref.shape
    length = ranks * rows
    half = cols // 2
    block = min(length, max(2 * STRETCH, length // 4))
    item = place_ref[0] * pl.num_programs(0) + pl.program_id(0)
    lam = lam_ref[lax.rem(item, lam_ref.shape[0])]
    gain = gain_ref[...]
    query = got_ref[:, 0, 0].reshape(length, cols)
    keys = got_ref[:, 0, 1].reshape(length, cols)
    values = got_ref[:, 0, 2].reshape(length, cols)
    values = jnp.concatenate([values, jnp.ones_like(values)], axis=1)
    first_map = lax.broadcasted_iota(jnp.int32, (block, cols), 1) < half
    row = lax.rem(lax.broadcasted_iota(jnp.int32, (2 * block, block), 0), block)
    col = lax.broadcasted_iota(jnp.int32, (2 * block, block), 1)
    visible = col // STRETCH <= row // STRETCH
    factor = LOG2E * half**-0.5
    for start in range(0, length, block):
        stop = start + block
        part = query[start:stop]
        zero = jnp.zeros_like(part)
        both = jnp.concatenate([jnp.where(first_map, part, zero), jnp.where(first_map, zero, part)], axis=0)
        near = jnp.where(visible, contract_last(both, keys[start:stop]), HIDDEN)
        top = jnp.max(near, axis=1, keepdims=True)
        if start:
            far = contract_last(both, keys[:start])
            top = jnp.maximum(top, jnp.max(far, axis=1, keepdims=True))
        mapped = jnp.dot(
            jnp.exp2((near - top) * factor).astype(jnp.bfloat16),
            values[start:stop],
            preferred_element_type=jnp.float32,
        )
        if start:
            mapped += jnp.dot(
                jnp.exp2((far - top) * factor).astype(jnp.bfloat16),
                values[:start],
                preferred_element_type=jnp.float32,
            )
        mapped = mapped[:, :cols] / mapped[:, cols:]
        combined = mapped[:block] - lam * mapped[block:]
        mean_sq = jnp.mean(combined * combined, axis=1, keepdims=True)
        normed = (combined * lax.rsqrt(mean_sq + EPS) * gain).astype(jnp.bfloat16)
        out_ref[start // rows : stop // rows, 0] = normed.reshape(block // rows, rows, cols)


def attend(got, mix_lambda, head_gain):
    ranks, items, _, rows, cols = got.shape
    place = lax.axis_index("sp").astype(jnp.int32)[None]
    return pl.pallas_call(
        attend_kernel,
        grid=(items,),
        out_shape=jax.ShapeDtypeStruct((ranks, items, rows, cols), jnp.bfloat16),
        in_specs=[
            pl.BlockSpec(memory_space=pltpu.SMEM),
            pl.BlockSpec(memory_space=pltpu.SMEM),
            pl.BlockSpec((1, cols), lambda i: (0, 0)),
            pl.BlockSpec((ranks, 1, 3, rows, cols), lambda i: (0, i, 0, 0, 0)),
        ],
        out_specs=pl.BlockSpec((ranks, 1, rows, cols), lambda i: (0, i, 0, 0)),
        cost_estimate=pl.CostEstimate(flops=6_000_000_000, bytes_accessed=4_000_000, transcendentals=0),
        name="attend",
    )(place, mix_lambda, head_gain[None, :], got)


def project_kernel(normed_ref, gate_ref, weight_ref, out_ref, gated_ref):
    seqs, heads, rows, cols = normed_ref.shape
    total = seqs * rows

    @pl.when(pl.program_id(0) == 0)
    def _():
        to = lax.broadcasted_iota(jnp.int32, (total, total), 0)
        of = lax.broadcasted_iota(jnp.int32, (total, total), 1)
        spread = (of == lax.rem(to, seqs) * rows + to // seqs).astype(jnp.bfloat16)
        for head in range(heads):
            span = slice(head * cols, (head + 1) * cols)
            by_seq = normed_ref[:, head].reshape(total, cols)
            by_token = jnp.dot(spread, by_seq, preferred_element_type=jnp.float32)
            gate = jax.nn.sigmoid(gate_ref[:, span].astype(jnp.float32))
            gated_ref[:, span] = (gate * by_token).astype(jnp.bfloat16)

    out_ref[...] = jnp.dot(gated_ref[...], weight_ref[0], preferred_element_type=jnp.float32).astype(jnp.bfloat16)


def project(normed, gate, weight):
    seqs, heads, rows, cols = normed.shape
    parts, depth, width = weight.shape
    total = seqs * rows
    return pl.pallas_call(
        project_kernel,
        grid=(parts,),
        out_shape=jax.ShapeDtypeStruct((total, parts * width), jnp.bfloat16),
        in_specs=[
            pl.BlockSpec((seqs, heads, rows, cols), lambda j: (0, 0, 0, 0)),
            pl.BlockSpec((total, depth), lambda j: (0, 0)),
            pl.BlockSpec((1, depth, width), lambda j: (j, 0, 0)),
        ],
        out_specs=pl.BlockSpec((total, width), lambda j: (0, j)),
        scratch_shapes=[pltpu.VMEM((total, depth), jnp.bfloat16)],
        cost_estimate=pl.CostEstimate(flops=2_000_000_000, bytes_accessed=10_000_000, transcendentals=0),
        name="project",
    )(normed, gate, weight)


def on_device(queries, key_maps, value_rows, gate_logits, mix_lambda, head_gain, out_weight):
    seqs, heads, rows, cols = queries.shape
    ranks = lax.axis_size("sp")
    items = seqs * heads // ranks
    width = gate_logits.shape[2]
    sent = jnp.stack([a.reshape(ranks, items, rows, cols) for a in (queries, key_maps, value_rows)], axis=2)
    got = lax.all_to_all(sent, "sp", split_axis=0, concat_axis=0, tiled=True)
    normed = attend(got, mix_lambda, head_gain)
    returned = lax.all_to_all(normed, "sp", split_axis=0, concat_axis=0, tiled=True)
    weight = lax.all_gather(out_weight, "sp", axis=0, tiled=True)
    weight = lax.all_gather(weight, "dp", axis=0, tiled=False)
    result = project(
        returned.reshape(seqs, heads, rows, cols), gate_logits.reshape(rows * seqs, width), weight
    )
    return result.reshape(rows, seqs, width)


def solution(mesh):
    placed = (
        P("dp", None, "sp", None),
        P("dp", None, "sp", None),
        P("dp", None, "sp", None),
        P("sp", "dp", None),
        P(),
        P(),
        P("sp", "dp"),
    )
    return jax.shard_map(
        on_device, mesh=mesh, in_specs=placed, out_specs=P("sp", "dp", None), check_vma=False
    )
```

```python
import functools
import math

import jax
import jax.numpy as jnp
from jax import lax
from jax.experimental import pallas as pl
from jax.experimental.pallas import tpu as pltpu
from jax.sharding import PartitionSpec as P

STRETCH = 64
EPS = 1e-05
HIDDEN = -1e30
LOG2E = math.log2(math.e)


def contract_last(a, b):
    return lax.dot_general(a, b, (((1,), (1,)), ((), ())), preferred_element_type=jnp.float32)


def attend_kernel(place_ref, lam_ref, gain_ref, got_ref, out_ref):
    ranks, _, _, rows, cols = got_ref.shape
    length = ranks * rows
    half = cols // 2
    block = min(length, max(2 * STRETCH, length // 4))
    item = place_ref[0] * pl.num_programs(0) + pl.program_id(0)
    lam = lam_ref[lax.rem(item, lam_ref.shape[0])]
    gain = gain_ref[...]
    query = got_ref[:, 0, 0].reshape(length, cols)
    keys = got_ref[:, 0, 1].reshape(length, cols)
    values = got_ref[:, 0, 2].reshape(length, cols)
    values = jnp.concatenate([values, jnp.ones_like(values)], axis=1)
    first_map = lax.broadcasted_iota(jnp.int32, (block, cols), 1) < half
    row = lax.rem(lax.broadcasted_iota(jnp.int32, (2 * block, block), 0), block)
    col = lax.broadcasted_iota(jnp.int32, (2 * block, block), 1)
    visible = col // STRETCH <= row // STRETCH
    factor = LOG2E * half**-0.5
    for start in range(0, length, block):
        stop = start + block
        part = query[start:stop]
        zero = jnp.zeros_like(part)
        both = jnp.concatenate([jnp.where(first_map, part, zero), jnp.where(first_map, zero, part)], axis=0)
        near = jnp.where(visible, contract_last(both, keys[start:stop]), HIDDEN)
        top = jnp.max(near, axis=1, keepdims=True)
        if start:
            far = contract_last(both, keys[:start])
            top = jnp.maximum(top, jnp.max(far, axis=1, keepdims=True))
        mapped = jnp.dot(
            jnp.exp2((near - top) * factor).astype(jnp.bfloat16),
            values[start:stop],
            preferred_element_type=jnp.float32,
        )
        if start:
            mapped += jnp.dot(
                jnp.exp2((far - top) * factor).astype(jnp.bfloat16),
                values[:start],
                preferred_element_type=jnp.float32,
            )
        mapped = mapped[:, :cols] / mapped[:, cols:]
        combined = mapped[:block] - lam * mapped[block:]
        mean_sq = jnp.mean(combined * combined, axis=1, keepdims=True)
        normed = (combined * lax.rsqrt(mean_sq + EPS) * gain).astype(jnp.bfloat16)
        out_ref[start // rows : stop // rows, 0] = normed.reshape(block // rows, rows, cols)


def attend(got, mix_lambda, head_gain):
    ranks, items, _, rows, cols = got.shape
    place = lax.axis_index("sp").astype(jnp.int32)[None]
    return pl.pallas_call(
        attend_kernel,
        grid=(items,),
        out_shape=jax.ShapeDtypeStruct((ranks, items, rows, cols), jnp.bfloat16),
        in_specs=[
            pl.BlockSpec(memory_space=pltpu.SMEM),
            pl.BlockSpec(memory_space=pltpu.SMEM),
            pl.BlockSpec((1, cols), lambda i: (0, 0)),
            pl.BlockSpec((ranks, 1, 3, rows, cols), lambda i: (0, i, 0, 0, 0)),
        ],
        out_specs=pl.BlockSpec((ranks, 1, rows, cols), lambda i: (0, i, 0, 0)),
        cost_estimate=pl.CostEstimate(flops=6_000_000_000, bytes_accessed=4_000_000, transcendentals=0),
        name="attend",
    )(place, mix_lambda, head_gain[None, :], got)


def project_kernel(place_ref, normed_ref, gate_ref, *refs):
    weight_refs, out_ref, gated_ref = refs[:-2], refs[-2], refs[-1]
    seqs, heads, rows, cols = normed_ref.shape
    total = seqs * rows
    to = lax.broadcasted_iota(jnp.int32, (total, total), 0)
    of = lax.broadcasted_iota(jnp.int32, (total, total), 1)
    spread = (of == lax.rem(to, seqs) * rows + to // seqs).astype(jnp.bfloat16)
    for head in range(heads):
        span = slice(head * cols, (head + 1) * cols)
        by_seq = normed_ref[:, head].reshape(total, cols)
        by_token = jnp.dot(spread, by_seq, preferred_element_type=jnp.float32)
        gate = jax.nn.sigmoid(gate_ref[:, span].astype(jnp.float32))
        gated_ref[:, span] = (gate * by_token).astype(jnp.bfloat16)
    for piece, weight_ref in enumerate(weight_refs):
        width = weight_ref.shape[1]
        start = pl.multiple_of(jnp.bitwise_xor(place_ref[0], piece) * width, width)
        out_ref[:, pl.ds(start, width)] = jnp.dot(
            gated_ref[...], weight_ref[...], preferred_element_type=jnp.float32
        ).astype(jnp.bfloat16)


def project(normed, gate, pieces):
    seqs, heads, rows, cols = normed.shape
    depth, width = pieces[0].shape
    total = seqs * rows
    vmem = pl.BlockSpec(memory_space=pltpu.VMEM)
    return pl.pallas_call(
        project_kernel,
        out_shape=jax.ShapeDtypeStruct((total, len(pieces) * width), jnp.bfloat16),
        in_specs=[pl.BlockSpec(memory_space=pltpu.SMEM)] + [vmem] * (2 + len(pieces)),
        out_specs=vmem,
        scratch_shapes=[pltpu.VMEM((total, depth), jnp.bfloat16)],
        cost_estimate=pl.CostEstimate(flops=2_000_000_000, bytes_accessed=10_000_000, transcendentals=0),
        name="project",
    )(lax.axis_index("dp").astype(jnp.int32)[None], normed, gate, *pieces)


def swap(array, axis, bit):
    return lax.ppermute(array, axis, [(i, i ^ bit) for i in range(lax.axis_size(axis))])


def gather_weight(block):
    ranks, parts = lax.axis_size("sp"), lax.axis_size("dp")
    me = lax.axis_index("sp")
    depth, width = block.shape
    held = block
    bits = ranks.bit_length() - 1
    for k in reversed(range(bits)):
        came = swap(held, "sp", 1 << k)
        upper = (me >> k) & 1 == 1
        held = jnp.stack([jnp.where(upper, came, held), jnp.where(upper, held, came)])
    held = jnp.transpose(held, tuple(reversed(range(bits))) + (bits, bits + 1))
    pieces = {0: held.reshape(ranks * depth, width)}
    bit = parts >> 1
    while bit:
        pieces.update({index ^ bit: swap(piece, "dp", bit) for index, piece in pieces.items()})
        bit >>= 1
    return [pieces[index] for index in range(parts)]


def on_device(queries, key_maps, value_rows, gate_logits, mix_lambda, head_gain, out_weight):
    seqs, heads, rows, cols = queries.shape
    ranks = lax.axis_size("sp")
    items = seqs * heads // ranks
    width = gate_logits.shape[2]
    pieces = gather_weight(out_weight)
    sent = jnp.stack([a.reshape(ranks, items, rows, cols) for a in (queries, key_maps, value_rows)], axis=2)
    got = lax.all_to_all(sent, "sp", split_axis=0, concat_axis=0, tiled=True)
    normed = attend(got, mix_lambda, head_gain)
    returned = lax.all_to_all(normed, "sp", split_axis=0, concat_axis=0, tiled=True)
    result = project(
        returned.reshape(seqs, heads, rows, cols), gate_logits.reshape(rows * seqs, width), pieces
    )
    return result.reshape(rows, seqs, width)


def solution(mesh):
    placed = (
        P("dp", None, "sp", None),
        P("dp", None, "sp", None),
        P("dp", None, "sp", None),
        P("sp", "dp", None),
        P(),
        P(),
        P("sp", "dp"),
    )
    return jax.shard_map(
        on_device, mesh=mesh, in_specs=placed, out_specs=P("sp", "dp", None), check_vma=False
    )
```
